32 devices in a mesh: sp: 8 (over z, y), fs: 2 (over x), tp: 2 (over core).
Axes of the slice: x: 2, y: 2, z: 4, core: 2. Of those that a mesh axis runs over, the one named last changes fastest.
Arguments:
- tokens: bfloat16 [8192, 2048], P(('fs', 'sp', 'tp')), parts along dimension 0, may hold values from -60 to 60
- norm_gain: float32 [2048], replicated, may hold values from 0.1 to 1.9
- pool_in: bfloat16 [2048, 512], P('sp', 'tp'), may hold values from -0.125 to 0.125
- gate_in: bfloat16 [2048, 1024], P('sp', 'tp'), may hold values from -0.125 to 0.125
- value_in: bfloat16 [2048, 1024], P('sp', 'tp'), may hold values from -0.125 to 0.125
- pool_mix: bfloat16 [4, 128, 128], P('tp'), may hold values from -0.5 to 0.5
- averaging_factor: float32 [512], P('tp'), may hold values from 0.25 to 0.75
- conv_taps: float32 [4, 1024], P(None, 'tp'), may hold values from -3 to 3
- rate_mix: bfloat16 [16, 64, 64], P('tp'), may hold values from -0.75 to 0.75
- input_mix: bfloat16 [16, 64, 64], P('tp'), may hold values from -0.75 to 0.75
- log_rate: float32 [1024], P('tp'), may hold values from 1.5 to 16
- decay_shift: float32 [32, 4096], P(('fs', 'tp'), 'sp'), parts along dimension 0, may hold values from -1.1 to 0
- initial_state: float32 [2048], P(('fs', 'tp')), parts along dimension 0, may hold values from -6 to 6
- out_pool: bfloat16 [2048, 512], P('sp', 'tp'), may hold values from -0.15625 to 0.15625
- out_rnn: bfloat16 [2048, 1024], P('sp', 'tp'), may hold values from -0.15625 to 0.15625
Outputs:
- mixed: bfloat16 [8192, 2048], P(('fs', 'sp', 'tp')), parts along dimension 0
The draws below stay inside these ranges and needn't reach their ends.
There are 2 independent parts, one for each index of `fs`. The reference program is written for one: setup_inputs(seed, part) draws one part's arguments, and reference() takes and returns one part's arrays. A program takes and returns all parts, laid end to end along the dimension named above; an argument that names none is the same for every part. Nothing has to cross between parts.
All inputs are finite; a program needn't handle non-finite values.
Results may differ from the reference program's by a relative error of at most 0.012.
Values may be sent and summed in bfloat16 or wider, within the bound.
A program may use at most 64 MiB of HBM per device.

```python
import math
import jax
import jax.numpy as jnp
from jax import lax

D = 2048
POOL = 512
GROUPS = 4
GROUP_WIDTH = 128
LOOP_BRANCHES = 16
HEAD_DIM = 64
RNN = 1024
TAPS = 4
REACH = 16
TOK_DEV = 512
TOKEN_COUNT = 4096


def draw_tokens(key, part):
    derived_seed_list = jax.random.split(key, 3)
    row_scales = jnp.exp(jax.random.uniform(derived_seed_list[0], (TOKEN_COUNT, 1), jnp.float32, math.log(0.5), math.log(5.0)))
    column_scales = jnp.exp(jax.random.uniform(derived_seed_list[1], (1, D), jnp.float32, math.log(0.3), math.log(3.0)))
    entries = jax.random.truncated_normal(derived_seed_list[2], -4.0, 4.0, (TOKEN_COUNT, D), jnp.float32)
    return (entries * row_scales * column_scales).astype(jnp.bfloat16)


def draw_log_rate(key, part):
    derived_seed_list = jax.random.split(key, 3)
    chance = 0.5
    fast_heads = jax.random.bernoulli(derived_seed_list[0], chance, (LOOP_BRANCHES,))
    fast_rate = jax.random.uniform(derived_seed_list[1], (RNN,), jnp.float32, 2.0, 4.0) / TOK_DEV
    slow_rate = jax.random.uniform(derived_seed_list[2], (RNN,), jnp.float32, 0.04, 0.12) / TOKEN_COUNT
    per_channel = jnp.repeat(fast_heads, HEAD_DIM)
    step_rate = jnp.where(per_channel, fast_rate, slow_rate)
    return -jnp.log(jnp.expm1(step_rate))


def draw_decay_shift(key, part):
    derived_seed_list = jax.random.split(key, 3)
    blocks = TOKEN_COUNT // TOK_DEV
    block_level = jnp.exp(jax.random.uniform(derived_seed_list[0], (LOOP_BRANCHES, blocks), jnp.float32, math.log(0.1), math.log(2.0))) / TOKEN_COUNT
    steady_signal = -jnp.repeat(block_level, TOK_DEV, axis=1)
    cluster_indices = jax.random.randint(derived_seed_list[1], (LOOP_BRANCHES, 2, 1), 0, TOKEN_COUNT)
    loss_values = jax.random.uniform(derived_seed_list[2], (LOOP_BRANCHES, 2, 1), jnp.float32, 0.2, 0.4)
    match_tests = jnp.arange(TOKEN_COUNT, dtype=jnp.int32)[None, None, :] == cluster_indices
    spike_events = jnp.sum(jnp.where(match_tests, jnp.log1p(-loss_values), 0.0), axis=1)
    return steady_signal + spike_events


def shard_levels(key, shape, cuts, smallest, largest):
    level, own = 1.0, jax.random.fold_in(key, 6)
    for axis_at, parts in cuts:
        draws = jnp.exp(jax.random.uniform(jax.random.fold_in(own, axis_at), (parts,), jnp.float32, smallest / len(cuts), largest / len(cuts)))
        level = level * jnp.repeat(draws, shape[axis_at] // parts).reshape([-1 if axis == axis_at else 1 for axis in range(len(shape))])
    return level


def centred(own_key, shape, width, bound, cuts=(), kind=jnp.bfloat16):
    result = width * jax.random.normal(own_key, shape, jnp.float32)
    if cuts:
        result = result * shard_levels(own_key, shape, cuts, -0.22, 0.18)
    return jnp.clip(result, -bound, bound).astype(kind)


def setup_inputs(seed: int = 0, part: int = 0) -> dict:
    arg_keys = jax.random.split(jax.random.key(seed), 16)
    part_keys = jax.random.split(jax.random.fold_in(arg_keys[15], part), 16)
    tokens = draw_tokens(jax.random.fold_in(jax.random.fold_in(arg_keys[15], part), 71), part)
    norm_gain = jnp.clip(1.0 + 0.18 * jax.random.normal(arg_keys[1], (D,), jnp.float32), 0.1, 1.9)
    pool_in = centred(arg_keys[2], (D, POOL), D ** -0.5, 0.125, ((0, 8), (1, 2)))
    gate_in = centred(arg_keys[3], (D, RNN), D ** -0.5, 0.125, ((0, 8), (1, 2)))
    value_in = centred(arg_keys[4], (D, RNN), D ** -0.5, 0.125, ((0, 8), (1, 2)))
    pool_mix = centred(arg_keys[5], (GROUPS, GROUP_WIDTH, GROUP_WIDTH), GROUP_WIDTH ** -0.5, 0.5, ((0, 2),))
    averaging_factor = jnp.clip(0.25 + 0.5 * jax.random.uniform(arg_keys[6], (POOL,), jnp.float32) ** shard_levels(arg_keys[6], (POOL,), ((0, 2),), -0.2, 0.2), 0.25, 0.75)
    conv_taps = centred(arg_keys[7], (TAPS, RNN), TAPS ** -0.5, 3.0, ((1, 2),), jnp.float32)
    rate_mix = centred(arg_keys[8], (LOOP_BRANCHES, HEAD_DIM, HEAD_DIM), HEAD_DIM ** -0.5, 0.75, ((0, 2),))
    input_mix = centred(arg_keys[9], (LOOP_BRANCHES, HEAD_DIM, HEAD_DIM), HEAD_DIM ** -0.5, 0.75, ((0, 2),))
    log_rate = draw_log_rate(jax.random.fold_in(arg_keys[15], 71), part)
    decay_shift = draw_decay_shift(jax.random.fold_in(jax.random.fold_in(arg_keys[15], part), 71), part)
    initial_state = centred(part_keys[12], (RNN,), 1.0, 6.0, ((0, 2),), jnp.float32)
    out_pool = centred(arg_keys[13], (D, POOL), (POOL + RNN) ** -0.5, 0.15625, ((0, 8), (1, 2)))
    out_rnn = centred(arg_keys[14], (D, RNN), (POOL + RNN) ** -0.5, 0.15625, ((0, 8), (1, 2)))
    return {"tokens": tokens, "norm_gain": norm_gain, "pool_in": pool_in, "gate_in": gate_in, "value_in": value_in, "pool_mix": pool_mix, "averaging_factor": averaging_factor, "conv_taps": conv_taps, "rate_mix": rate_mix, "input_mix": input_mix, "log_rate": log_rate, "decay_shift": decay_shift, "initial_state": initial_state, "out_pool": out_pool, "out_rnn": out_rnn}


epsilon = 1e-06
sharpness = 8.0

def chain_pairs(first_pair, second_pair):
    return (first_pair[0] * second_pair[0], second_pair[0] * first_pair[1] + second_pair[1])

def reference(tokens, norm_gain, pool_in, gate_in, value_in, pool_mix, averaging_factor, conv_taps, rate_mix, input_mix, log_rate, decay_shift, initial_state, out_pool, out_rnn):
    widened = tokens.astype(jnp.float32)
    scaling = lax.rsqrt(lax.optimization_barrier(jnp.mean(widened * widened, axis=1, keepdims=True)) + epsilon)
    normed = (widened * scaling * norm_gain[None, :]).astype(jnp.bfloat16)
    pool_pre = jnp.dot(normed, pool_in, preferred_element_type=jnp.float32).astype(jnp.bfloat16)
    gate_pre = jnp.dot(normed, gate_in, preferred_element_type=jnp.float32).astype(jnp.bfloat16)
    value_pre = jnp.dot(normed, value_in, preferred_element_type=jnp.float32).astype(jnp.bfloat16)
    pool_values = pool_pre.astype(jnp.float32)
    pool_padded = jnp.pad(pool_values, ((REACH, 0), (0, 0)))
    positions = jnp.arange(TOKEN_COUNT, dtype=jnp.int32)
    pieces = []
    for group_index in range(GROUPS):
        window = 2 ** (group_index + 1)
        low_column = group_index * GROUP_WIDTH
        high_column = low_column + GROUP_WIDTH
        window_sum = jnp.zeros((TOKEN_COUNT, GROUP_WIDTH), jnp.float32)
        for steps_back in range(window):
            window_sum = window_sum + pool_padded[REACH - steps_back:REACH - steps_back + TOKEN_COUNT, low_column:high_column]
        counts = jnp.minimum(positions + 1, window).astype(jnp.float32)[:, None]
        pieces.append(window_sum / counts - pool_values[:, low_column:high_column])
    pooled = jnp.concatenate(pieces, axis=1).astype(jnp.bfloat16)
    mixed_groups = jnp.einsum('tgc,gcd->tgd', pooled.reshape(TOKEN_COUNT, GROUPS, GROUP_WIDTH).astype(jnp.float32), pool_mix.astype(jnp.float32))
    pool_out = (mixed_groups.reshape(TOKEN_COUNT, POOL) * averaging_factor[None, :]).astype(jnp.bfloat16)
    value_padded = jnp.pad(value_pre.astype(jnp.float32), ((TAPS - 1, 0), (0, 0)))
    convolved = conv_taps[0][None, :] * value_padded[0:TOKEN_COUNT]
    for tap_index in range(1, TAPS):
        convolved = convolved + conv_taps[tap_index][None, :] * value_padded[tap_index:tap_index + TOKEN_COUNT]
    conv_out = convolved.astype(jnp.bfloat16)
    conv_heads = conv_out.reshape(TOKEN_COUNT, LOOP_BRANCHES, HEAD_DIM).astype(jnp.float32)
    rate_gate = jax.nn.sigmoid(jnp.einsum('thc,hcd->thd', conv_heads, rate_mix.astype(jnp.float32))).reshape(TOKEN_COUNT, RNN)
    input_gate = jax.nn.sigmoid(jnp.einsum('thc,hcd->thd', conv_heads, input_mix.astype(jnp.float32))).reshape(TOKEN_COUNT, RNN)
    shifts = jnp.broadcast_to(jnp.transpose(decay_shift)[:, :, None], (TOKEN_COUNT, LOOP_BRANCHES, HEAD_DIM)).reshape(TOKEN_COUNT, RNN)
    log_decay = -sharpness * rate_gate * jax.nn.softplus(-log_rate)[None, :] + shifts
    decays = jnp.exp(log_decay)
    drives = jnp.sqrt(-jnp.expm1(2.0 * log_decay)) * input_gate * conv_out.astype(jnp.float32)
    cumulative, local_state = lax.associative_scan(chain_pairs, (decays, drives), axis=0)
    hidden_state = local_state + cumulative * initial_state[None, :]
    rnn_out = (jax.nn.gelu(gate_pre.astype(jnp.float32), approximate=True) * hidden_state).astype(jnp.bfloat16)
    pool_term = jnp.dot(pool_out, jnp.transpose(out_pool), preferred_element_type=jnp.float32)
    rnn_term = jnp.dot(rnn_out, jnp.transpose(out_rnn), preferred_element_type=jnp.float32)
    return (pool_term + rnn_term).astype(jnp.bfloat16)
```

```python
import functools

import jax
import jax.numpy as jnp
from jax import lax
from jax.experimental import pallas as pl
from jax.experimental.pallas import tpu as pltpu
from jax.sharding import PartitionSpec as P

GROUP_WIDTH = 128
HEAD_DIM = 64
TAPS = 4
REACH = 16
LANES = 128
TILE = 16
MESH = pl.DeviceIdType.MESH

epsilon = 1e-06
sharpness = 8.0


def sigmoid(x):
    return 1.0 / (1.0 + jnp.exp(-x))


def softplus(v):
    small = jnp.exp(-jnp.abs(v))
    above = 1.0 + small
    gap = above - 1.0
    safe = jnp.where(gap == 0.0, 1.0, gap)
    log1p = jnp.where(gap == 0.0, small, jnp.log(above) * small / safe)
    return jnp.maximum(v, 0.0) + log1p


def one_minus_exp(y, exp_y):
    series = 1.0 + y * (1.0 / 8.0)
    for k in range(7, 1, -1):
        series = 1.0 + y * (1.0 / k) * series
    return jnp.where(y > -0.5, -y * series, 1.0 - exp_y)


def gelu(x):
    return 0.5 * x * (1.0 + jnp.tanh(0.7978845608028654 * (x + 0.044715 * x * x * x)))


def layer(
    sizes,
    tokens, gain, pool_in, gate_in, value_in, pool_mix, averaging, taps, rate_mix, input_mix,
    log_rate, shift, initial, out_pool, out_rnn,
    o_ref,
    other_tokens, normed, held_in, held_out, acc, ppad, vpad, edge_out, edge_got, cum, loc,
    ends, ends_got, mix, own_sum, sum_out, sum_got,
    local_sem, ring_send, ring_recv, cross_send, cross_recv, tok_sem, edge_sem,
    end_send, end_recv, sum_send, sum_recv,
):
    n, fs, tp = sizes
    s = lax.axis_index("sp")
    f = lax.axis_index("fs")
    t = lax.axis_index("tp")
    depth = pool_in.shape[0]
    pool_width = pool_in.shape[1]
    rnn_width = gate_in.shape[1]
    half_rows = tokens.shape[0]
    rows = half_rows * tp
    other = 1 - t
    if n % 2 == 0:
        place = jnp.where(s % 2 == 0, s // 2, n - 1 - s // 2)

        def at_place(p):
            p = (p + 2 * n) % n
            return jnp.where(p < n // 2, 2 * p, 2 * (n - 1 - p) + 1)
    else:
        place = s

        def at_place(p):
            return (p + 2 * n) % n

    right, left = at_place(place + 1), at_place(place - 1)
    crossing = fs == 2
    if crossing:
        part = depth // 3 // TILE * TILE
        common = depth - 2 * part
        e_start = pl.multiple_of(f * (part + common), TILE)
        x_start = pl.multiple_of((1 - f) * (part + common), TILE)
        a_start = part
    else:
        part = depth // 2
        common = depth - part
        e_start, a_start, x_start = 0, part, 0
    pieces = (pl.ds(e_start, part), pl.ds(a_start, common))
    far = n // 2
    pending = []

    barrier = pltpu.get_barrier_semaphore()
    copies = []
    for k, (src, dst) in enumerate((
        (pool_in, held_in.at[s, :, pl.ds(0, pool_width)]),
        (gate_in, held_in.at[s, :, pl.ds(pool_width, rnn_width)]),
        (value_in, held_in.at[s, :, pl.ds(pool_width + rnn_width, rnn_width)]),
        (out_pool, held_out.at[s, :, pl.ds(0, pool_width)]),
        (out_rnn, held_out.at[s, :, pl.ds(pool_width, rnn_width)]),
    )):
        copy = pltpu.make_async_copy(src, dst, local_sem.at[k])
        copy.start()
        copies.append(copy)
    for k in range(1, n):
        pl.semaphore_signal(barrier, inc=1, device_id={"sp": (s + k) % n}, device_id_type=MESH)
    pl.semaphore_signal(barrier, inc=1, device_id={"tp": other}, device_id_type=MESH)
    if crossing:
        pl.semaphore_signal(barrier, inc=1, device_id={"fs": 1 - f}, device_id_type=MESH)
    pl.semaphore_wait(barrier, n + (1 if crossing else 0))

    held = (held_in, held_out)

    def carried(d, way):
        if 2 * d == n:
            return (way,)
        return (0, 1)

    def send(stream, d, way, piece, block):
        ref = held[stream].at[block, pieces[piece], :]
        copy = pltpu.make_async_remote_copy(
            src_ref=ref, dst_ref=ref,
            send_sem=ring_send.at[stream, d, way, piece],
            recv_sem=ring_recv.at[stream, d, way, piece],
            device_id={"sp": right if way == 0 else left}, device_id_type=MESH,
        )
        copy.start()
        pending.append(copy)

    def ring_descriptor(stream, d, way, piece, block):
        ref = held[stream].at[block, pieces[piece], :]
        return pltpu.make_async_remote_copy(
            src_ref=ref, dst_ref=ref,
            send_sem=ring_send.at[stream, d, way, piece],
            recv_sem=ring_recv.at[stream, d, way, piece],
            device_id={"sp": right if way == 0 else left}, device_id_type=MESH,
        )

    def block_at(d, way):
        return at_place(place - d) if way == 0 else at_place(place + d)

    def start_ring(stream):
        for piece in (0, 1):
            for way in (0, 1):
                if piece in carried(1, way):
                    send(stream, 1, way, piece, s)

    def ring_step(stream, d):
        for piece in (0, 1):
            for way in (0, 1):
                if piece not in carried(d, way):
                    continue
                block = block_at(d, way)
                ring_descriptor(stream, d, way, piece, block).wait_recv()
                if d < far and piece in carried(d + 1, way):
                    send(stream, d + 1, way, piece, block)
                if crossing and piece == 0:
                    ref = held[stream].at[block, pieces[0], :]
                    copy = pltpu.make_async_remote_copy(
                        src_ref=ref, dst_ref=ref,
                        send_sem=cross_send.at[stream, d, way],
                        recv_sem=cross_recv.at[stream, d, way],
                        device_id={"fs": 1 - f}, device_id_type=MESH,
                    )
                    copy.start()
                    pending.append(copy)

    def blocks_of(stream, d):
        result = []
        for way in (0, 1):
            if 2 * d == n and way == 1:
                continue
            block = block_at(d, way)
            if crossing:
                ref = held[stream].at[block, pl.ds(x_start, part), :]
                pltpu.make_async_remote_copy(
                    src_ref=ref, dst_ref=ref,
                    send_sem=cross_send.at[stream, d, way],
                    recv_sem=cross_recv.at[stream, d, way],
                    device_id={"fs": 1 - f}, device_id_type=MESH,
                ).wait_recv()
            result.append(block)
        return result

    for copy in copies[:3]:
        copy.wait()
    if far:
        start_ring(0)
    token_copy = pltpu.make_async_remote_copy(
        src_ref=tokens, dst_ref=other_tokens, send_sem=tok_sem.at[0], recv_sem=tok_sem.at[1],
        device_id={"tp": other}, device_id_type=MESH,
    )
    token_copy.start()
    pending.append(token_copy)
    for copy in copies[3:]:
        copy.wait()

    step_rows = 32

    def normalize(source, base):
        @pl.loop(0, half_rows // step_rows)
        def _(i):
            at = pl.multiple_of(i * step_rows, step_rows)
            wide = source[pl.ds(at, step_rows), :].astype(jnp.float32)
            scale = lax.rsqrt(jnp.mean(wide * wide, axis=1, keepdims=True) + epsilon)
            result = (wide * scale * gain[...]).astype(jnp.bfloat16)
            put = pl.ds(pl.multiple_of(base + at, step_rows), step_rows)
            for b in range(n):
                normed[b, put, :] = result[:, b * depth : (b + 1) * depth]

    normalize(tokens, t * half_rows)
    token_copy.wait_recv()
    normalize(other_tokens, other * half_rows)

    total_width = acc.shape[1]
    wide_step = 256 if total_width % 256 == 0 else LANES

    def project(block, first=False):
        @pl.loop(0, total_width // wide_step)
        def _(j):
            cols = pl.ds(pl.multiple_of(j * wide_step, wide_step), wide_step)
            product = jnp.dot(
                normed[block], held_in[block, :, cols], preferred_element_type=jnp.float32
            )
            if first:
                acc[:, cols] = product
            else:
                acc[:, cols] += product

    project(s, True)
    for d in range(1, far + 1):
        if d == far:
            start_ring(1)
        ring_step(0, d)
        if d > 1:
            for block in blocks_of(0, d - 1):
                project(block)
    if far:
        for block in blocks_of(0, far):
            project(block)

    advanced = [0]

    def advance():
        if advanced[0] < far:
            advanced[0] += 1
            ring_step(1, advanced[0])

    last = pl.ds(rows - REACH, REACH)
    edge_out[:, pl.ds(0, pool_width)] = acc[last, pl.ds(0, pool_width)].astype(jnp.bfloat16)
    edge_out[:, pl.ds(pool_width, rnn_width)] = acc[
        last, pl.ds(pool_width + rnn_width, rnn_width)
    ].astype(jnp.bfloat16)
    edge_copy = pltpu.make_async_remote_copy(
        src_ref=edge_out, dst_ref=edge_got, send_sem=edge_sem.at[0], recv_sem=edge_sem.at[1],
        device_id={"sp": (s + 1) % n}, device_id_type=MESH,
    )
    edge_copy.start()
    pending.append(edge_copy)

    here = pl.ds(REACH, rows)
    for c in range(pool_width // LANES):
        cols = pl.ds(c * LANES, LANES)
        ppad[here, cols] = acc[:, cols].astype(jnp.bfloat16).astype(jnp.float32)
    for c in range(rnn_width // LANES):
        vpad[here, pl.ds(c * LANES, LANES)] = (
            acc[:, pl.ds(pool_width + rnn_width + c * LANES, LANES)]
            .astype(jnp.bfloat16).astype(jnp.float32)
        )
    edge_copy.wait_recv()
    begins = s > 0
    ppad[pl.ds(0, REACH), :] = jnp.where(
        begins, edge_got[:, pl.ds(0, pool_width)].astype(jnp.float32), 0.0
    )
    vpad[pl.ds(0, REACH), :] = jnp.where(
        begins, edge_got[:, pl.ds(pool_width, rnn_width)].astype(jnp.float32), 0.0
    )

    row_at = lax.broadcasted_iota(jnp.int32, (rows, LANES), 0)
    ends[...] = jnp.zeros_like(ends)

    @pl.loop(0, rnn_width // LANES)
    def _(c):
        cols = pl.ds(pl.multiple_of(c * LANES, LANES), LANES)
        padded = vpad[:, cols]
        conv = taps[TAPS - 1 : TAPS, cols] * padded[REACH:]
        for back in range(1, TAPS):
            conv = conv + taps[TAPS - 1 - back : TAPS - back, cols] * pltpu.roll(padded, back, 0)[REACH:]
        conv = conv.astype(jnp.bfloat16)
        wide = conv.astype(jnp.float32)
        r_at = lax.broadcasted_iota(jnp.int32, (HEAD_DIM, LANES), 0)
        c_at = lax.broadcasted_iota(jnp.int32, (HEAD_DIM, LANES), 1)
        repeat = jnp.where((c_at - r_at) % HEAD_DIM == 0, 1.0, 0.0).astype(jnp.bfloat16)
        same = (
            lax.broadcasted_iota(jnp.int32, (LANES, LANES), 0) // HEAD_DIM
            == lax.broadcasted_iota(jnp.int32, (LANES, LANES), 1) // HEAD_DIM
        )

        def gate_of(matrix):
            spread = jnp.dot(matrix[cols, :], repeat, preferred_element_type=jnp.float32)
            diagonal = jnp.where(same, spread, 0.0).astype(jnp.bfloat16)
            return sigmoid(jnp.dot(conv, diagonal, preferred_element_type=jnp.float32))

        rate = gate_of(rate_mix)
        per = LANES // HEAD_DIM
        lane_head = lax.broadcasted_iota(jnp.int32, (LANES, rows), 0) // HEAD_DIM
        across = jnp.broadcast_to(shift[pl.ds(c * per, 1), :], (LANES, rows))
        for k in range(1, per):
            across = jnp.where(lane_head == k, shift[pl.ds(c * per + k, 1), :], across)
        log_decay = -sharpness * rate * softplus(-log_rate[:, cols]) + jnp.transpose(across)
        a = jnp.exp(log_decay)
        b = jnp.sqrt(one_minus_exp(2.0 * log_decay, a * a)) * gate_of(input_mix) * wide
        step = 1
        while step < rows:
            if step < 8:
                reached = row_at >= step
                before_a = jnp.where(reached, pltpu.roll(a, step, 0), 1.0)
                before_b = jnp.where(reached, pltpu.roll(b, step, 0), 0.0)
            else:
                before_a = jnp.concatenate([jnp.ones((step, LANES), jnp.float32), a[:-step]], axis=0)
                before_b = jnp.concatenate([jnp.zeros((step, LANES), jnp.float32), b[:-step]], axis=0)
            b = b + a * before_b
            a = a * before_a
            step *= 2
        cum[:, cols] = a
        loc[:, cols] = b
        ends[0:1, cols] = a[rows - 1 : rows]
        ends[1:2, cols] = b[rows - 1 : rows]

    for k in range(1, n):
        copy = pltpu.make_async_remote_copy(
            src_ref=ends, dst_ref=ends_got.at[k], send_sem=end_send.at[k], recv_sem=end_recv.at[k],
            device_id={"sp": (s + k) % n}, device_id_type=MESH,
        )
        copy.start()
        pending.append(copy)
    advance()

    groups_here = pool_width // GROUP_WIDTH
    positions = s * rows + row_at
    for g in range(groups_here):
        cols = pl.ds(g * GROUP_WIDTH, GROUP_WIDTH)
        group = t * groups_here + g
        padded = ppad[:, cols]
        value = padded[REACH:]
        total = padded
        window_sum = jnp.zeros_like(value)
        window = 1
        k = 0
        while 2 ** (k + 1) <= REACH:
            total = total + pltpu.roll(total, 2**k, 0)
            window_sum = jnp.where(group == k, total[REACH:], window_sum)
            window = jnp.where(group == k, 2 ** (k + 1), window)
            k += 1
        counts = jnp.minimum(positions + 1, window).astype(jnp.float32)
        pooled = (window_sum / counts - value).astype(jnp.bfloat16)
        mixed = jnp.dot(pooled, pool_mix[g], preferred_element_type=jnp.float32)
        mix[:, cols] = (mixed * averaging[:, cols]).astype(jnp.bfloat16)
    advance()

    carry = initial[...]
    for k in range(n - 1, 0, -1):
        pltpu.make_async_remote_copy(
            src_ref=ends, dst_ref=ends_got.at[k], send_sem=end_send.at[k], recv_sem=end_recv.at[k],
            device_id={"sp": (s + k) % n}, device_id_type=MESH,
        ).wait_recv()
        carry = jnp.where(k <= s, ends_got[k, 0:1, :] * carry + ends_got[k, 1:2, :], carry)

    for c in range(rnn_width // LANES):
        cols = pl.ds(c * LANES, LANES)
        hidden = loc[:, cols] + cum[:, cols] * carry[:, c * LANES : (c + 1) * LANES]
        gate = acc[:, pl.ds(pool_width + c * LANES, LANES)].astype(jnp.bfloat16).astype(jnp.float32)
        mix[:, pl.ds(pool_width + c * LANES, LANES)] = (gelu(gate) * hidden).astype(jnp.bfloat16)
    advance()

    mine = pl.ds(pl.multiple_of(t * half_rows, half_rows), half_rows)
    theirs = pl.ds(pl.multiple_of(other * half_rows, half_rows), half_rows)
    dims = (((1,), (1,)), ((), ()))
    sums = []

    def sum_copy(i, block):
        return pltpu.make_async_remote_copy(
            src_ref=sum_out.at[block], dst_ref=sum_got.at[block],
            send_sem=sum_send.at[i], recv_sem=sum_recv.at[i],
            device_id={"tp": other}, device_id_type=MESH,
        )

    def produce(block):
        i = len(sums)
        sum_out[block] = lax.dot_general(
            mix[theirs, :], held_out[block], dims, preferred_element_type=jnp.float32
        ).astype(jnp.bfloat16)
        copy = sum_copy(i, block)
        copy.start()
        pending.append(copy)
        sums.append(block)
        own_sum[block] = lax.dot_general(
            mix[mine, :], held_out[block], dims, preferred_element_type=jnp.float32
        )

    produce(s)
    for d in range(1, far + 1):
        if d > advanced[0]:
            advance()
        for block in blocks_of(1, d):
            produce(block)
    aligned = depth % LANES == 0
    for i, block in enumerate(sums):
        sum_copy(i, block).wait_recv()
        if aligned:
            o_ref[:, pl.ds(pl.multiple_of(block * depth, LANES), depth)] = (
                own_sum[block] + sum_got[block].astype(jnp.float32)
            ).astype(jnp.bfloat16)
    if not aligned:
        for b in range(n):
            o_ref[:, b * depth : (b + 1) * depth] = (
                own_sum[b] + sum_got[b].astype(jnp.float32)
            ).astype(jnp.bfloat16)
    for copy in pending:
        copy.wait_send()


def shards(
    sizes,
    tokens, norm_gain, pool_in, gate_in, value_in, pool_mix, averaging_factor, conv_taps,
    rate_mix, input_mix, log_rate, decay_shift, initial_state, out_pool, out_rnn,
):
    n, fs, tp = sizes
    half_rows, width = tokens.shape
    rows = half_rows * tp
    depth, pool_width = pool_in.shape
    rnn_width = gate_in.shape[1]
    bf, f32 = jnp.bfloat16, jnp.float32
    far = n // 2
    vmem = pl.BlockSpec(memory_space=pltpu.VMEM)
    hbm = pl.BlockSpec(memory_space=pl.ANY)
    dma = pltpu.SemaphoreType.DMA
    all_in = pool_width + 2 * rnn_width
    all_out = pool_width + rnn_width
    return pl.pallas_call(
        functools.partial(layer, sizes),
        out_shape=jax.ShapeDtypeStruct((half_rows, width), bf),
        in_specs=[vmem, vmem, hbm, hbm, hbm, vmem, vmem, vmem, vmem, vmem, vmem, vmem, vmem, hbm, hbm],
        out_specs=vmem,
        scratch_shapes=[
            pltpu.VMEM((half_rows, width), bf),
            pltpu.VMEM((n, rows, depth), bf),
            pltpu.VMEM((n, depth, all_in), bf),
            pltpu.VMEM((n, depth, all_out), bf),
            pltpu.VMEM((rows, all_in), f32),
            pltpu.VMEM((REACH + rows, pool_width), f32),
            pltpu.VMEM((REACH + rows, rnn_width), f32),
            pltpu.VMEM((REACH, all_out), bf),
            pltpu.VMEM((REACH, all_out), bf),
            pltpu.VMEM((rows, rnn_width), f32),
            pltpu.VMEM((rows, rnn_width), f32),
            pltpu.VMEM((8, rnn_width), f32),
            pltpu.VMEM((n, 8, rnn_width), f32),
            pltpu.VMEM((rows, all_out), bf),
            pltpu.VMEM((n, half_rows, depth), f32),
            pltpu.VMEM((n, half_rows, depth), bf),
            pltpu.VMEM((n, half_rows, depth), bf),
            dma((5,)),
            dma((2, far + 1, 2, 2)),
            dma((2, far + 1, 2, 2)),
            dma((2, far + 1, 2)),
            dma((2, far + 1, 2)),
            dma((2,)),
            dma((2,)),
            dma((n,)),
            dma((n,)),
            dma((n,)),
            dma((n,)),
        ],
        compiler_params=pltpu.CompilerParams(
            collective_id=0, has_side_effects=True, vmem_limit_bytes=60 * 1024 * 1024
        ),
    )(
        tokens,
        norm_gain[None, :],
        pool_in,
        gate_in,
        value_in,
        pool_mix,
        averaging_factor[None, :],
        conv_taps,
        rate_mix.reshape(rnn_width, HEAD_DIM),
        input_mix.reshape(rnn_width, HEAD_DIM),
        log_rate[None, :],
        decay_shift,
        initial_state[None, :],
        out_pool,
        out_rnn,
    )


def solution(mesh):
    sizes = (mesh.shape["sp"], mesh.shape["fs"], mesh.shape["tp"])
    placed = (
        P(("fs", "sp", "tp"), None),
        P(),
        P("sp", "tp"),
        P("sp", "tp"),
        P("sp", "tp"),
        P("tp", None, None),
        P("tp"),
        P(None, "tp"),
        P("tp", None, None),
        P("tp", None, None),
        P("tp"),
        P(("fs", "tp"), "sp"),
        P(("fs", "tp")),
        P("sp", "tp"),
        P("sp", "tp"),
    )
    return jax.shard_map(
        functools.partial(shards, sizes),
        mesh=mesh,
        in_specs=placed,
        out_specs=P(("fs", "sp", "tp"), None),
        check_vma=False,
    )
```

```python
import functools

import jax
import jax.numpy as jnp
from jax import lax
from jax.experimental import pallas as pl
from jax.experimental.pallas import tpu as pltpu
from jax.sharding import PartitionSpec as P

GROUP_WIDTH = 128
HEAD_DIM = 64
TAPS = 4
REACH = 16
LANES = 128
TILE = 16
MESH = pl.DeviceIdType.MESH

epsilon = 1e-06
sharpness = 8.0


def sigmoid(x):
    return 1.0 / (1.0 + jnp.exp(-x))


def softplus(v):
    small = jnp.exp(-jnp.abs(v))
    above = 1.0 + small
    gap = above - 1.0
    safe = jnp.where(gap == 0.0, 1.0, gap)
    log1p = jnp.where(gap == 0.0, small, jnp.log(above) * small / safe)
    return jnp.maximum(v, 0.0) + log1p


def one_minus_exp(y, exp_y):
    series = 1.0 + y * (1.0 / 8.0)
    for k in range(7, 1, -1):
        series = 1.0 + y * (1.0 / k) * series
    return jnp.where(y > -0.5, -y * series, 1.0 - exp_y)


def gelu(x):
    return 0.5 * x * (1.0 + jnp.tanh(0.7978845608028654 * (x + 0.044715 * x * x * x)))


def layer(
    sizes,
    tokens_hbm, gain_hbm, pool_in, gate_in, value_in, pool_mix_hbm, averaging_hbm, taps_hbm,
    rate_mix_hbm, input_mix_hbm, log_rate_hbm, shift_hbm, initial_hbm, out_pool, out_rnn,
    result_hbm,
    tokens, gain, pool_mix, averaging, taps, rate_mix, input_mix, log_rate, shift, initial, o_ref,
    other_tokens, normed, held_in, held_out, acc, ppad, vpad, edge_out, edge_got, cum, loc,
    ends, ends_got, mix, own_sum, sum_out, sum_got,
    local_sem, result_sem, ring_send, ring_recv, cross_send, cross_recv, tok_sem, edge_sem,
    end_send, end_recv, sum_send, sum_recv,
):
    n, fs, tp = sizes
    s = lax.axis_index("sp")
    f = lax.axis_index("fs")
    t = lax.axis_index("tp")
    depth = pool_in.shape[0]
    pool_width = pool_in.shape[1]
    rnn_width = gate_in.shape[1]
    half_rows = tokens.shape[0]
    rows = half_rows * tp
    other = 1 - t
    if n % 2 == 0:
        place = jnp.where(s % 2 == 0, s // 2, n - 1 - s // 2)

        def at_place(p):
            p = (p + 2 * n) % n
            return jnp.where(p < n // 2, 2 * p, 2 * (n - 1 - p) + 1)
    else:
        place = s

        def at_place(p):
            return (p + 2 * n) % n

    right, left = at_place(place + 1), at_place(place - 1)
    crossing = fs == 2
    if crossing:
        part = depth // 3 // TILE * TILE
        common = depth - 2 * part
        e_start = pl.multiple_of(f * (part + common), TILE)
        x_start = pl.multiple_of((1 - f) * (part + common), TILE)
        a_start = part
    else:
        part = depth // 2
        common = depth - part
        e_start, a_start, x_start = 0, part, 0
    pieces = (pl.ds(e_start, part), pl.ds(a_start, common))
    far = n // 2
    pending = []

    barrier = pltpu.get_barrier_semaphore()
    for neighbour in (left, right):
        pl.semaphore_signal(barrier, inc=1, device_id={"sp": neighbour}, device_id_type=MESH)
    pl.semaphore_signal(barrier, inc=1, device_id={"tp": other}, device_id_type=MESH)
    if crossing:
        pl.semaphore_signal(barrier, inc=1, device_id={"fs": 1 - f}, device_id_type=MESH)
    copies = []
    for k, (src, dst) in enumerate((
        (pool_in, held_in.at[s, :, pl.ds(0, pool_width)]),
        (gate_in, held_in.at[s, :, pl.ds(pool_width, rnn_width)]),
        (value_in, held_in.at[s, :, pl.ds(pool_width + rnn_width, rnn_width)]),
        (tokens_hbm, tokens),
        (gain_hbm, gain),
        (out_pool, held_out.at[s, :, pl.ds(0, pool_width)]),
        (out_rnn, held_out.at[s, :, pl.ds(pool_width, rnn_width)]),
        (pool_mix_hbm, pool_mix),
        (averaging_hbm, averaging),
        (taps_hbm, taps),
        (rate_mix_hbm, rate_mix),
        (input_mix_hbm, input_mix),
        (log_rate_hbm, log_rate),
        (shift_hbm, shift),
        (initial_hbm, initial),
    )):
        copy = pltpu.make_async_copy(src, dst, local_sem.at[k])
        copy.start()
        copies.append(copy)
    pl.semaphore_wait(barrier, 4 if crossing else 3)

    held = (held_in, held_out)

    def carried(d, way):
        if 2 * d == n:
            return (way,)
        return (0, 1)

    def send(stream, d, way, piece, block):
        ref = held[stream].at[block, pieces[piece], :]
        copy = pltpu.make_async_remote_copy(
            src_ref=ref, dst_ref=ref,
            send_sem=ring_send.at[stream, d, way, piece],
            recv_sem=ring_recv.at[stream, d, way, piece],
            device_id={"sp": right if way == 0 else left}, device_id_type=MESH,
        )
        copy.start()
        pending.append(copy)

    def ring_descriptor(stream, d, way, piece, block):
        ref = held[stream].at[block, pieces[piece], :]
        return pltpu.make_async_remote_copy(
            src_ref=ref, dst_ref=ref,
            send_sem=ring_send.at[stream, d, way, piece],
            recv_sem=ring_recv.at[stream, d, way, piece],
            device_id={"sp": right if way == 0 else left}, device_id_type=MESH,
        )

    def block_at(d, way):
        return at_place(place - d) if way == 0 else at_place(place + d)

    def start_ring(stream):
        for piece in (0, 1):
            for way in (0, 1):
                if piece in carried(1, way):
                    send(stream, 1, way, piece, s)

    def ring_step(stream, d):
        for piece in (0, 1):
            for way in (0, 1):
                if piece not in carried(d, way):
                    continue
                block = block_at(d, way)
                ring_descriptor(stream, d, way, piece, block).wait_recv()
                if d < far and piece in carried(d + 1, way):
                    send(stream, d + 1, way, piece, block)
                if crossing and piece == 0:
                    ref = held[stream].at[block, pieces[0], :]
                    copy = pltpu.make_async_remote_copy(
                        src_ref=ref, dst_ref=ref,
                        send_sem=cross_send.at[stream, d, way],
                        recv_sem=cross_recv.at[stream, d, way],
                        device_id={"fs": 1 - f}, device_id_type=MESH,
                    )
                    copy.start()
                    pending.append(copy)

    def blocks_of(stream, d):
        result = []
        for way in (0, 1):
            if 2 * d == n and way == 1:
                continue
            block = block_at(d, way)
            if crossing:
                ref = held[stream].at[block, pl.ds(x_start, part), :]
                pltpu.make_async_remote_copy(
                    src_ref=ref, dst_ref=ref,
                    send_sem=cross_send.at[stream, d, way],
                    recv_sem=cross_recv.at[stream, d, way],
                    device_id={"fs": 1 - f}, device_id_type=MESH,
                ).wait_recv()
            result.append(block)
        return result

    for copy in copies[:3]:
        copy.wait()
    if far:
        start_ring(0)
    for copy in copies[3:5]:
        copy.wait()
    token_copy = pltpu.make_async_remote_copy(
        src_ref=tokens, dst_ref=other_tokens, send_sem=tok_sem.at[0], recv_sem=tok_sem.at[1],
        device_id={"tp": other}, device_id_type=MESH,
    )
    token_copy.start()
    pending.append(token_copy)

    step_rows = 32

    def normalize(source, base):
        @pl.loop(0, half_rows // step_rows)
        def _(i):
            at = pl.multiple_of(i * step_rows, step_rows)
            wide = source[pl.ds(at, step_rows), :].astype(jnp.float32)
            scale = lax.rsqrt(jnp.mean(wide * wide, axis=1, keepdims=True) + epsilon)
            result = (wide * scale * gain[...]).astype(jnp.bfloat16)
            put = pl.ds(pl.multiple_of(base + at, step_rows), step_rows)
            for b in range(n):
                normed[b, put, :] = result[:, b * depth : (b + 1) * depth]

    normalize(tokens, t * half_rows)
    token_copy.wait_recv()
    normalize(other_tokens, other * half_rows)

    total_width = acc.shape[1]
    wide_step = 256 if total_width % 256 == 0 else LANES

    def project(block, first=False):
        @pl.loop(0, total_width // wide_step)
        def _(j):
            cols = pl.ds(pl.multiple_of(j * wide_step, wide_step), wide_step)
            product = jnp.dot(
                normed[block], held_in[block, :, cols], preferred_element_type=jnp.float32
            )
            if first:
                acc[:, cols] = product
            else:
                acc[:, cols] += product

    project(s, True)
    for copy in copies[5:]:
        copy.wait()
    for d in range(1, far + 1):
        if d == far:
            start_ring(1)
        ring_step(0, d)
        if d > 1:
            for block in blocks_of(0, d - 1):
                project(block)
    if far:
        for block in blocks_of(0, far):
            project(block)

    advanced = [0]

    def advance():
        if advanced[0] < far:
            advanced[0] += 1
            ring_step(1, advanced[0])

    last = pl.ds(rows - REACH, REACH)
    edge_out[:, pl.ds(0, pool_width)] = acc[last, pl.ds(0, pool_width)].astype(jnp.bfloat16)
    edge_out[:, pl.ds(pool_width, rnn_width)] = acc[
        last, pl.ds(pool_width + rnn_width, rnn_width)
    ].astype(jnp.bfloat16)
    edge_copy = pltpu.make_async_remote_copy(
        src_ref=edge_out, dst_ref=edge_got, send_sem=edge_sem.at[0], recv_sem=edge_sem.at[1],
        device_id={"sp": (s + 1) % n}, device_id_type=MESH,
    )
    edge_copy.start()
    pending.append(edge_copy)

    here = pl.ds(REACH, rows)
    for c in range(pool_width // LANES):
        cols = pl.ds(c * LANES, LANES)
        ppad[here, cols] = acc[:, cols].astype(jnp.bfloat16).astype(jnp.float32)
    for c in range(rnn_width // LANES):
        vpad[here, pl.ds(c * LANES, LANES)] = (
            acc[:, pl.ds(pool_width + rnn_width + c * LANES, LANES)]
            .astype(jnp.bfloat16).astype(jnp.float32)
        )
    edge_copy.wait_recv()
    begins = s > 0
    ppad[pl.ds(0, REACH), :] = jnp.where(
        begins, edge_got[:, pl.ds(0, pool_width)].astype(jnp.float32), 0.0
    )
    vpad[pl.ds(0, REACH), :] = jnp.where(
        begins, edge_got[:, pl.ds(pool_width, rnn_width)].astype(jnp.float32), 0.0
    )

    row_at = lax.broadcasted_iota(jnp.int32, (rows, LANES), 0)
    ends[...] = jnp.zeros_like(ends)

    def recur(c):
        cols = pl.ds(pl.multiple_of(c * LANES, LANES), LANES)
        padded = vpad[:, cols]
        conv = taps[TAPS - 1 : TAPS, cols] * padded[REACH:]
        for back in range(1, TAPS):
            conv = conv + taps[TAPS - 1 - back : TAPS - back, cols] * pltpu.roll(padded, back, 0)[REACH:]
        conv = conv.astype(jnp.bfloat16)
        wide = conv.astype(jnp.float32)
        r_at = lax.broadcasted_iota(jnp.int32, (HEAD_DIM, LANES), 0)
        c_at = lax.broadcasted_iota(jnp.int32, (HEAD_DIM, LANES), 1)
        repeat = jnp.where((c_at - r_at) % HEAD_DIM == 0, 1.0, 0.0).astype(jnp.bfloat16)
        same = (
            lax.broadcasted_iota(jnp.int32, (LANES, LANES), 0) // HEAD_DIM
            == lax.broadcasted_iota(jnp.int32, (LANES, LANES), 1) // HEAD_DIM
        )

        def gate_of(matrix):
            spread = jnp.dot(matrix[cols, :], repeat, preferred_element_type=jnp.float32)
            diagonal = jnp.where(same, spread, 0.0).astype(jnp.bfloat16)
            return sigmoid(jnp.dot(conv, diagonal, preferred_element_type=jnp.float32))

        rate = gate_of(rate_mix)
        per = LANES // HEAD_DIM
        lane_head = lax.broadcasted_iota(jnp.int32, (LANES, rows), 0) // HEAD_DIM
        across = jnp.broadcast_to(shift[pl.ds(c * per, 1), :], (LANES, rows))
        for k in range(1, per):
            across = jnp.where(lane_head == k, shift[pl.ds(c * per + k, 1), :], across)
        log_decay = -sharpness * rate * softplus(-log_rate[:, cols]) + jnp.transpose(across)
        a = jnp.exp(log_decay)
        b = jnp.sqrt(one_minus_exp(2.0 * log_decay, a * a)) * gate_of(input_mix) * wide
        step = 1
        while step < rows:
            if step < 8:
                reached = row_at >= step
                before_a = jnp.where(reached, pltpu.roll(a, step, 0), 1.0)
                before_b = jnp.where(reached, pltpu.roll(b, step, 0), 0.0)
            else:
                before_a = jnp.concatenate([jnp.ones((step, LANES), jnp.float32), a[:-step]], axis=0)
                before_b = jnp.concatenate([jnp.zeros((step, LANES), jnp.float32), b[:-step]], axis=0)
            b = b + a * before_b
            a = a * before_a
            step *= 2
        cum[:, cols] = a
        loc[:, cols] = b
        ends[0:1, cols] = a[rows - 1 : rows]
        ends[1:2, cols] = b[rows - 1 : rows]

    chunks = rnn_width // LANES
    pl.loop(0, chunks // 2)(recur)
    advance()
    pl.loop(chunks // 2, chunks)(recur)

    for k in range(1, n):
        copy = pltpu.make_async_remote_copy(
            src_ref=ends, dst_ref=ends_got.at[k], send_sem=end_send.at[k], recv_sem=end_recv.at[k],
            device_id={"sp": (s + k) % n}, device_id_type=MESH,
        )
        copy.start()
        pending.append(copy)
    advance()

    groups_here = pool_width // GROUP_WIDTH
    positions = s * rows + row_at
    for g in range(groups_here):
        cols = pl.ds(g * GROUP_WIDTH, GROUP_WIDTH)
        group = t * groups_here + g
        padded = ppad[:, cols]
        value = padded[REACH:]
        total = padded
        window_sum = jnp.zeros_like(value)
        window = 1
        k = 0
        while 2 ** (k + 1) <= REACH:
            total = total + pltpu.roll(total, 2**k, 0)
            window_sum = jnp.where(group == k, total[REACH:], window_sum)
            window = jnp.where(group == k, 2 ** (k + 1), window)
            k += 1
        counts = jnp.minimum(positions + 1, window).astype(jnp.float32)
        pooled = (window_sum / counts - value).astype(jnp.bfloat16)
        mixed = jnp.dot(pooled, pool_mix[g], preferred_element_type=jnp.float32)
        mix[:, cols] = (mixed * averaging[:, cols]).astype(jnp.bfloat16)
    advance()

    carry = initial[...]
    for k in range(n - 1, 0, -1):
        pltpu.make_async_remote_copy(
            src_ref=ends, dst_ref=ends_got.at[k], send_sem=end_send.at[k], recv_sem=end_recv.at[k],
            device_id={"sp": (s + k) % n}, device_id_type=MESH,
        ).wait_recv()
        carry = jnp.where(k <= s, ends_got[k, 0:1, :] * carry + ends_got[k, 1:2, :], carry)

    for c in range(rnn_width // LANES):
        cols = pl.ds(c * LANES, LANES)
        hidden = loc[:, cols] + cum[:, cols] * carry[:, c * LANES : (c + 1) * LANES]
        gate = acc[:, pl.ds(pool_width + c * LANES, LANES)].astype(jnp.bfloat16).astype(jnp.float32)
        mix[:, pl.ds(pool_width + c * LANES, LANES)] = (gelu(gate) * hidden).astype(jnp.bfloat16)
    advance()

    mine = pl.ds(pl.multiple_of(t * half_rows, half_rows), half_rows)
    theirs = pl.ds(pl.multiple_of(other * half_rows, half_rows), half_rows)
    dims = (((1,), (1,)), ((), ()))
    sums = []

    def sum_copy(i, block):
        return pltpu.make_async_remote_copy(
            src_ref=sum_out.at[block], dst_ref=sum_got.at[block],
            send_sem=sum_send.at[i], recv_sem=sum_recv.at[i],
            device_id={"tp": other}, device_id_type=MESH,
        )

    def produce(block):
        i = len(sums)
        sum_out[block] = lax.dot_general(
            mix[theirs, :], held_out[block], dims, preferred_element_type=jnp.float32
        ).astype(jnp.bfloat16)
        copy = sum_copy(i, block)
        copy.start()
        pending.append(copy)
        sums.append(block)
        own_sum[block] = lax.dot_general(
            mix[mine, :], held_out[block], dims, preferred_element_type=jnp.float32
        )

    produce(s)
    for d in range(1, far + 1):
        if d > advanced[0]:
            advance()
        for block in blocks_of(1, d):
            produce(block)
    aligned = depth % LANES == 0
    results = []
    for i, block in enumerate(sums):
        sum_copy(i, block).wait_recv()
        if aligned:
            o_ref[:, pl.ds(pl.multiple_of(block * depth, LANES), depth)] = (
                own_sum[block] + sum_got[block].astype(jnp.float32)
            ).astype(jnp.bfloat16)
            columns = pl.ds(pl.multiple_of(block * depth, LANES), depth)
            copy = pltpu.make_async_copy(
                o_ref.at[:, columns], result_hbm.at[:, columns], result_sem.at[i]
            )
            copy.start()
            results.append(copy)
    if not aligned:
        for b in range(n):
            o_ref[:, b * depth : (b + 1) * depth] = (
                own_sum[b] + sum_got[b].astype(jnp.float32)
            ).astype(jnp.bfloat16)
        copy = pltpu.make_async_copy(o_ref, result_hbm, result_sem.at[0])
        copy.start()
        results.append(copy)
    for copy in pending:
        copy.wait_send()
    for copy in results:
        copy.wait()


def shards(
    sizes,
    tokens, norm_gain, pool_in, gate_in, value_in, pool_mix, averaging_factor, conv_taps,
    rate_mix, input_mix, log_rate, decay_shift, initial_state, out_pool, out_rnn,
):
    n, fs, tp = sizes
    half_rows, width = tokens.shape
    rows = half_rows * tp
    depth, pool_width = pool_in.shape
    rnn_width = gate_in.shape[1]
    bf, f32 = jnp.bfloat16, jnp.float32
    far = n // 2
    hbm = pl.BlockSpec(memory_space=pl.ANY)
    dma = pltpu.SemaphoreType.DMA
    all_in = pool_width + 2 * rnn_width
    all_out = pool_width + rnn_width
    return pl.pallas_call(
        functools.partial(layer, sizes),
        out_shape=jax.ShapeDtypeStruct((half_rows, width), bf),
        in_specs=[hbm] * 15,
        out_specs=hbm,
        scratch_shapes=[
            pltpu.VMEM((half_rows, width), bf),
            pltpu.VMEM((1, width), f32),
            pltpu.VMEM(pool_mix.shape, bf),
            pltpu.VMEM((1, pool_width), f32),
            pltpu.VMEM(conv_taps.shape, f32),
            pltpu.VMEM((rnn_width, HEAD_DIM), bf),
            pltpu.VMEM((rnn_width, HEAD_DIM), bf),
            pltpu.VMEM((1, rnn_width), f32),
            pltpu.VMEM(decay_shift.shape, f32),
            pltpu.VMEM((1, rnn_width), f32),
            pltpu.VMEM((half_rows, width), bf),
            pltpu.VMEM((half_rows, width), bf),
            pltpu.VMEM((n, rows, depth), bf),
            pltpu.VMEM((n, depth, all_in), bf),
            pltpu.VMEM((n, depth, all_out), bf),
            pltpu.VMEM((rows, all_in), f32),
            pltpu.VMEM((REACH + rows, pool_width), f32),
            pltpu.VMEM((REACH + rows, rnn_width), f32),
            pltpu.VMEM((REACH, all_out), bf),
            pltpu.VMEM((REACH, all_out), bf),
            pltpu.VMEM((rows, rnn_width), f32),
            pltpu.VMEM((rows, rnn_width), f32),
            pltpu.VMEM((8, rnn_width), f32),
            pltpu.VMEM((n, 8, rnn_width), f32),
            pltpu.VMEM((rows, all_out), bf),
            pltpu.VMEM((n, half_rows, depth), f32),
            pltpu.VMEM((n, half_rows, depth), bf),
            pltpu.VMEM((n, half_rows, depth), bf),
            dma((15,)),
            dma((n,)),
            dma((2, far + 1, 2, 2)),
            dma((2, far + 1, 2, 2)),
            dma((2, far + 1, 2)),
            dma((2, far + 1, 2)),
            dma((2,)),
            dma((2,)),
            dma((n,)),
            dma((n,)),
            dma((n,)),
            dma((n,)),
        ],
        compiler_params=pltpu.CompilerParams(
            collective_id=0, has_side_effects=True, vmem_limit_bytes=60 * 1024 * 1024
        ),
    )(
        tokens,
        norm_gain[None, :],
        pool_in,
        gate_in,
        value_in,
        pool_mix,
        averaging_factor[None, :],
        conv_taps,
        rate_mix.reshape(rnn_width, HEAD_DIM),
        input_mix.reshape(rnn_width, HEAD_DIM),
        log_rate[None, :],
        decay_shift,
        initial_state[None, :],
        out_pool,
        out_rnn,
    )


def solution(mesh):
    sizes = (mesh.shape["sp"], mesh.shape["fs"], mesh.shape["tp"])
    placed = (
        P(("fs", "sp", "tp"), None),
        P(),
        P("sp", "tp"),
        P("sp", "tp"),
        P("sp", "tp"),
        P("tp", None, None),
        P("tp"),
        P(None, "tp"),
        P("tp", None, None),
        P("tp", None, None),
        P("tp"),
        P(("fs", "tp"), "sp"),
        P(("fs", "tp")),
        P("sp", "tp"),
        P("sp", "tp"),
    )
    return jax.shard_map(
        functools.partial(shards, sizes),
        mesh=mesh,
        in_specs=placed,
        out_specs=P(("fs", "sp", "tp"), None),
        check_vma=False,
    )
```
